32 devices in a mesh: ep: 8 (over z, core), tp: 4 (over y, x).
Axes of the slice: x: 2, y: 2, z: 4, core: 2. Of those that a mesh axis runs over, the one named last changes fastest.
Arguments:
- mix_rows: bfloat16 [2048, 2048], P('ep', 'tp'), may hold values from -6 to 6
- mix_gain: bfloat16 [2048], replicated, may hold values from 0.099609375 to 1.8984375
- w_query: bfloat16 [2048, 2048], P(None, 'tp'), may hold values from -0.125 to 0.125
- w_forget: bfloat16 [2048, 2048], P(None, 'tp'), may hold values from -0.125 to 0.125
- w_input: bfloat16 [2048, 2048], P(None, 'tp'), may hold values from -0.125 to 0.125
- w_outgate: bfloat16 [2048, 2048], P(None, 'tp'), may hold values from -0.125 to 0.125
- forget_gap: float32 [2048], P('tp'), may hold values from 1e-05 to 0.1
- decay_extra: float32 [16, 2048], P('tp', 'ep'), may hold values from -0.7 to 0, as said below
- head_gain: bfloat16 [128], replicated, may hold values from 0.099609375 to 1.8984375
- w_mixout: bfloat16 [2048, 2048], P('tp'), may hold values from -0.125 to 0.125
- moe_rows: bfloat16 [2048, 2048], P('ep', 'tp'), may hold values from -6 to 6
- moe_gain: bfloat16 [2048], replicated, may hold values from 0.099609375 to 1.8984375
- route_ids: int32 [2048, 2], P('ep'), may hold values from 0 to 7, all different within a row; in each aligned block of 256 rows (0 to 255, 256 to 511, ...) at most 96 rows name the same one
- route_scores: float32 [2048, 2], P('ep'), may hold values from 0.05 to 1
- w_gate: bfloat16 [8, 2048, 3072], P('ep', None, 'tp'), may hold values from -0.125 to 0.125
- w_up: bfloat16 [8, 2048, 3072], P('ep', None, 'tp'), may hold values from -0.125 to 0.125
- w_down: bfloat16 [8, 3072, 2048], P('ep', 'tp'), may hold values from -0.109375 to 0.109375
Outputs:
- mix_out: bfloat16 [2048, 2048], P('ep', 'tp')
- moe_out: bfloat16 [2048, 2048], P('ep', 'tp')
The draws below stay inside these ranges and needn't reach their ends.
Inputs may be any that keep to these rules, and one draw needn't show every extreme that they name: `route_ids`: each row names 2 different experts. Among the rows of one index of ep at most 96 name the same expert, a bound that at least one block reaches. `decay_extra`: never positive.
All inputs are finite; a program needn't handle non-finite values.
Results may differ from the reference program's by a relative error of at most 0.017.
Values may be sent and summed in bfloat16 or wider, within the bound.
No kernel may reach another device: no remote copies, remote signals or barrier semaphores. Data moves between devices by JAX's collectives and lax.ppermute only.
A program may use at most 64 MiB of HBM per device.

```python
import math
import jax
import jax.numpy as jnp
import numpy as np
from jax import lax

HEADS = 16
HEAD_DIM = 128
D = 2048
FFE = 3072
EXPERTS = 8
TOP_K = 2
BLOCK = 64
TOK_A = 256
TOK_B = 256
TOKENS_A = 2048
TOKENS_B = 2048
CAP = 96
N_EP = 8
N_TP = 4


def draw_forget_gap(key, part):
    lowest, highest = (1e-05, 0.1)
    unit = jax.random.uniform(key, (D,), jnp.float32)
    return jnp.exp(jnp.log(lowest) + unit * (jnp.log(highest) - jnp.log(lowest)))


def draw_decay_extra(key, part):
    rate_key, spot_key, depth_key = jax.random.split(key, 3)
    lowest, highest = (1e-05, 0.0001)
    block_list = TOKENS_A // TOK_A
    unit = jax.random.uniform(rate_key, (HEADS, block_list, 1), jnp.float32)
    rate = jnp.exp(jnp.log(lowest) + unit * (jnp.log(highest) - jnp.log(lowest)))
    steady = jnp.broadcast_to(-rate, (HEADS, block_list, TOK_A)).reshape(HEADS, TOKENS_A)
    spots = jax.random.randint(spot_key, (3,), 0, TOKENS_A)
    marked = jnp.any(jnp.arange(TOKENS_A)[None, :] == spots[:, None], axis=0)
    depth = jnp.log(jax.random.uniform(depth_key, (HEADS, TOKENS_A), jnp.float32, 0.5, 0.8))
    return steady + jnp.where(marked[None, :], depth, 0.0)


def block_scale(rng, extent, cuts, smallest, largest):
    factor_of = 1.0
    for position, shards_of in cuts:
        draws = jax.random.uniform(jax.random.fold_in(jax.random.fold_in(rng, 6), position), (shards_of,), jnp.float32, smallest / len(cuts), largest / len(cuts))
        factor_of = factor_of * jnp.repeat(jnp.exp(draws), extent[position] // shards_of).reshape((-1,) + (1,) * (len(extent) - 1 - position))
    return factor_of


def assign_block(key, own, number, rows, amount, top, limit, skew):
    ranking = jax.random.permutation(key, amount)
    crowded, common = load_shares(amount, rows * top, limit, skew, True), load_shares(amount, rows * top, limit, skew, False)
    places = jnp.arange(amount)

    def named(tallies, offset_by):
        used = int((tallies > 0).sum())
        fixed = max(1, used // 4)
        moved = fixed + (places - fixed + offset_by * (used - fixed)) % max(1, amount - fixed)
        return jnp.zeros((amount,), jnp.int32).at[ranking[jnp.where(places < fixed, places, moved)]].set(jnp.asarray(tallies, jnp.int32))

    tallies = jnp.where(number % 4 == 0, named(crowded, number // 4), named(common, number - number // 4 - 1))
    mixed = jax.random.permutation(jax.random.fold_in(own, 3), amount)
    source_of, taker = mixed[0:amount // 2 * 2:2], mixed[1:amount // 2 * 2:2]
    margin = jnp.minimum(tallies[source_of] - 1, limit - tallies[taker]) // 2
    margin = jnp.where((source_of == ranking[0]) | (taker == ranking[0]) | (tallies[taker] == 0), 0, jnp.maximum(margin, 0))
    moved = jax.random.randint(jax.random.fold_in(own, 4), (amount // 2,), 0, 1 << 20) % (margin + 1)
    tallies = tallies.at[source_of].add(-moved).at[taker].add(moved)
    members = jnp.searchsorted(jnp.cumsum(tallies), jnp.arange(rows * top), side="right").astype(jnp.int32)
    table = members.reshape(top, rows).T
    table = table[jax.random.permutation(jax.random.fold_in(own, 1), rows)]
    offset_by = jax.random.randint(jax.random.fold_in(own, 2), (rows, 1), 0, top)
    return jnp.take_along_axis(table, (jnp.arange(top)[None, :] + offset_by) % top, axis=1)


def load_shares(count, total, limit, skew, full):
    portions = [(1 << 20) // math.isqrt(standing ** skew) + 1 for standing in range(1, count + 1)]
    largest = limit if full else min(limit, max(-(-total // count), total * portions[0] // sum(portions)))
    least = 1 if total - largest >= count - 1 else 0
    counts, surplus = [largest] + [least] * (count - 1), total - largest - least * (count - 1)
    while surplus > 0:
        candidates = [i for i in range(1, count) if counts[i] < largest] or [i for i in range(1, count) if counts[i] < limit]
        mass, remaining = sum([portions[i] for i in candidates]), surplus
        for i in candidates:
            addition = min(limit - counts[i], max(1, remaining * portions[i] // mass), surplus)
            counts[i] = counts[i] + addition
            surplus = surplus - addition
    return np.array(counts)


def bell_draw(stream_key, extent, scale, bound, shards=(), held_as=jnp.bfloat16):
    loudness = block_scale(stream_key, extent, shards, -0.22, 0.18) if shards else 1.0
    drawn = jax.random.normal(stream_key, extent, jnp.float32) * scale * loudness
    return jnp.minimum(jnp.maximum(drawn, -bound), bound).astype(held_as)


def setup_inputs(seed: int = 0) -> dict:
    splits = jax.random.split(jax.random.key(seed), 18)
    mix_rows = bell_draw(splits[0], (TOKENS_A, D), 1.0, 6.0, ((0, 8), (1, 4)))
    mix_gain = jnp.clip(1.0 + 0.18 * jax.random.normal(splits[1], (D,), jnp.float32), 0.099609375, 1.8984375).astype(jnp.bfloat16)
    w_query = bell_draw(splits[2], (D, D), D ** -0.5, 0.125, ((1, 4),))
    w_forget = bell_draw(splits[3], (D, D), D ** -0.5, 0.125, ((1, 4),))
    w_input = bell_draw(splits[4], (D, D), D ** -0.5, 0.125, ((1, 4),))
    w_outgate = bell_draw(splits[5], (D, D), D ** -0.5, 0.125, ((1, 4),))
    forget_gap = draw_forget_gap(jax.random.fold_in(splits[17], 71), 0)
    decay_extra = draw_decay_extra(jax.random.fold_in(splits[17], 71), 0)
    head_gain = jnp.clip(1.0 + 0.18 * jax.random.normal(splits[8], (HEAD_DIM,), jnp.float32), 0.099609375, 1.8984375).astype(jnp.bfloat16)
    w_mixout = bell_draw(splits[9], (D, D), D ** -0.5, 0.125, ((0, 4),))
    moe_rows = bell_draw(splits[10], (TOKENS_B, D), 1.0, 6.0, ((0, 8), (1, 4)))
    moe_gain = jnp.clip(1.0 + 0.18 * jax.random.normal(splits[11], (D,), jnp.float32), 0.099609375, 1.8984375).astype(jnp.bfloat16)
    route_ids_keys = jax.random.split(jax.random.fold_in(splits[12], 1), TOKENS_B // TOK_B)
    route_ids_turns = jax.random.permutation(jax.random.fold_in(splits[12], 3), TOKENS_B // TOK_B)
    route_ids = jax.vmap(lambda own, number: assign_block(jax.random.fold_in(splits[12], 2), own, number, TOK_B, EXPERTS, TOP_K, CAP, 1))(route_ids_keys, route_ids_turns).reshape((TOKENS_B, TOP_K))
    route_scores = jnp.clip(0.05 + 0.95 * jax.random.uniform(splits[13], (TOKENS_B, TOP_K), jnp.float32) ** block_scale(splits[13], (TOKENS_B, TOP_K), ((0, 8),), -0.2, 0.2), 0.05, 1.0)
    w_gate = bell_draw(splits[14], (EXPERTS, D, FFE), D ** -0.5, 0.125, ((0, 8), (2, 4)))
    w_up = bell_draw(splits[15], (EXPERTS, D, FFE), D ** -0.5, 0.125, ((0, 8), (2, 4)))
    w_down = bell_draw(splits[16], (EXPERTS, FFE, D), FFE ** -0.5, 0.109375, ((0, 8), (1, 4)))
    return dict(mix_rows=mix_rows, mix_gain=mix_gain, w_query=w_query, w_forget=w_forget, w_input=w_input, w_outgate=w_outgate, forget_gap=forget_gap, decay_extra=decay_extra, head_gain=head_gain, w_mixout=w_mixout, moe_rows=moe_rows, moe_gain=moe_gain, route_ids=route_ids, route_scores=route_scores, w_gate=w_gate, w_up=w_up, w_down=w_down)


epsilon = 1e-06
HIGHEST_PRECISION = lax.Precision.HIGHEST

def rms_scale(rows, gain):
    values = rows.astype(jnp.float32)
    scale = lax.rsqrt(lax.optimization_barrier(jnp.mean(values * values, axis=-1, keepdims=True)) + epsilon)
    return values * scale * gain.astype(jnp.float32)

def block_recurrence(query_rows, key_in, value, log_forget, state):
    heads_count, length, key_dim = query_rows.shape
    block_list = length // BLOCK

    def split(values):
        return jnp.moveaxis(values.reshape(heads_count, block_list, BLOCK, values.shape[2]), 1, 0)
    causal = jnp.tril(jnp.ones((BLOCK, BLOCK), dtype=bool))[:, :, None]

    def advance(carry, inputs):
        query_block, key_block, value_block, forget_block = inputs
        running_state = jnp.cumsum(forget_block, axis=1)
        spread = running_state[:, :, None, :] - running_state[:, None, :, :]
        decay = jnp.exp(jnp.where(causal, spread, -jnp.inf))
        scores = jnp.einsum('hid,hjd,hijd->hij', query_block, key_block, decay, precision=HIGHEST_PRECISION)
        output = jnp.einsum('hid,hde->hie', query_block * jnp.exp(running_state), carry, precision=HIGHEST_PRECISION)
        output = output + jnp.einsum('hij,hje->hie', scores, value_block, precision=HIGHEST_PRECISION)
        last = running_state[:, -1:, :]
        carry = carry * jnp.exp(last)[:, 0, :, None] + jnp.einsum('hjd,hje->hde', key_block * jnp.exp(last - running_state), value_block, precision=HIGHEST_PRECISION)
        return (carry, output)
    carry, outputs = lax.scan(advance, state, (split(query_rows), split(key_in), split(value), split(log_forget)))
    return (jnp.moveaxis(outputs, 0, 1).reshape(heads_count, length, value.shape[2]), carry)

def token_mixer(mix_rows, mix_gain, w_query, w_forget, w_input, w_outgate, forget_gap, decay_extra, head_gain, w_mixout):
    normed = rms_scale(mix_rows, mix_gain).astype(jnp.bfloat16)
    length = normed.shape[0]
    query_preactivation = jnp.dot(normed, w_query, preferred_element_type=jnp.float32)
    forget_pre = jnp.dot(normed, w_forget, preferred_element_type=jnp.float32)
    input_pre = jnp.dot(normed, w_input, preferred_element_type=jnp.float32)
    outgate_pre = jnp.dot(normed, w_outgate, preferred_element_type=jnp.float32)

    def heads(values):
        return values.reshape(length, HEADS, HEAD_DIM).transpose(1, 0, 2)
    query_rows = heads(jax.nn.silu(query_preactivation))
    key_in = heads(forget_gap.astype(jnp.float32) * jax.nn.sigmoid(-forget_pre))
    value = heads(input_pre)
    log_forget = jnp.log1p(-key_in) + decay_extra.astype(jnp.float32)[:, :, None]
    start_state = jnp.zeros((HEADS, HEAD_DIM, HEAD_DIM), jnp.float32)
    head_out, _ = block_recurrence(query_rows, key_in, value, log_forget, start_state)
    gated = rms_scale(head_out, head_gain) * heads(jax.nn.silu(outgate_pre))
    gated = gated.transpose(1, 0, 2).reshape(length, D).astype(jnp.bfloat16)
    group = D // N_TP
    total = jnp.zeros((length, D), jnp.float32)
    for index in range(N_TP):
        part = jnp.dot(gated[:, index * group:(index + 1) * group], w_mixout[index * group:(index + 1) * group], preferred_element_type=jnp.float32)
        total = total + lax.optimization_barrier(part.astype(jnp.bfloat16)).astype(jnp.float32)
    return total.astype(jnp.bfloat16)

def expert_layer(moe_rows, moe_gain, route_ids, route_scores, w_gate, w_up, w_down):
    row_total, top_count = route_ids.shape
    expert_count = w_gate.shape[0]
    normed = rms_scale(moe_rows, moe_gain).astype(jnp.bfloat16)
    weights = route_scores / lax.optimization_barrier(jnp.sum(route_scores, axis=1, keepdims=True))
    grouped = route_ids.reshape(N_EP, TOK_B * top_count).astype(jnp.int32)
    onehot = (grouped[:, :, None] == jnp.arange(expert_count, dtype=jnp.int32)[None, None, :]).astype(jnp.int32)
    rank = lax.optimization_barrier(jnp.sum((jnp.cumsum(onehot, axis=1) - 1) * onehot, axis=2)).astype(jnp.int32)
    source = jnp.arange(N_EP, dtype=jnp.int32)[:, None]
    place = (grouped * (N_EP * CAP) + source * CAP + rank).reshape(-1).astype(jnp.int32)
    token = (jnp.arange(row_total * top_count, dtype=jnp.int32) // top_count).astype(jnp.int32)
    table = jnp.full((expert_count * N_EP * CAP,), row_total, jnp.int32).at[place].set(token)
    padded = jnp.concatenate([normed, jnp.zeros((1, D), jnp.bfloat16)], axis=0)
    slots = padded[table].reshape(expert_count, N_EP * CAP, D)
    width = FFE // N_TP

    def one_expert(operands):
        rows, gate_weight, up_weight, down_weight = operands
        gate_acts = jnp.dot(rows, gate_weight, preferred_element_type=jnp.float32)
        up_acts = jnp.dot(rows, up_weight, preferred_element_type=jnp.float32)
        hidden = (jax.nn.silu(gate_acts) * up_acts).astype(jnp.bfloat16)
        total = jnp.zeros((rows.shape[0], D), jnp.float32)
        for index in range(N_TP):
            part = jnp.dot(hidden[:, index * width:(index + 1) * width], down_weight[index * width:(index + 1) * width], preferred_element_type=jnp.float32)
            total = total + lax.optimization_barrier(part.astype(jnp.bfloat16)).astype(jnp.float32)
        return total.astype(jnp.bfloat16)
    results = lax.map(one_expert, (slots, w_gate, w_up, w_down)).reshape(-1, D)
    picked = results[place].astype(jnp.float32).reshape(row_total, top_count, D)
    return lax.optimization_barrier(jnp.sum(picked * weights[:, :, None], axis=1)).astype(jnp.bfloat16)

def reference(mix_rows, mix_gain, w_query, w_forget, w_input, w_outgate, forget_gap, decay_extra, head_gain, w_mixout, moe_rows, moe_gain, route_ids, route_scores, w_gate, w_up, w_down):
    mix_out = token_mixer(mix_rows, mix_gain, w_query, w_forget, w_input, w_outgate, forget_gap, decay_extra, head_gain, w_mixout)
    moe_out = expert_layer(moe_rows, moe_gain, route_ids, route_scores, w_gate, w_up, w_down)
    return (mix_out, moe_out)
```

```python
import functools

import jax
import jax.numpy as jnp
from jax import lax
from jax.experimental import pallas as pl
from jax.experimental.pallas import tpu as pltpu
from jax.sharding import PartitionSpec as P

BLOCK = 64
EPS = 1e-06
F32 = jnp.float32
BF16 = jnp.bfloat16


def dot(a, b, dims=((1,), (0,)), precision=None):
    return lax.dot_general(a, b, (dims, ((), ())), precision=precision, preferred_element_type=F32)


def whole(shape):
    return pl.BlockSpec(shape, lambda *_: (0,) * len(shape))


def params(n=1):
    return pltpu.CompilerParams(dimension_semantics=("arbitrary",) * n, vmem_limit_bytes=48 * 1024 * 1024)


def call(kernel, scalars, grid, in_specs, out_specs, out_shape, scratch, cost, name, args):
    return pl.pallas_call(
        kernel,
        grid_spec=pltpu.PrefetchScalarGridSpec(
            num_scalar_prefetch=1, grid=grid, in_specs=in_specs, out_specs=out_specs, scratch_shapes=scratch
        ),
        out_shape=out_shape,
        compiler_params=params(len(grid)),
        cost_estimate=pl.CostEstimate(flops=cost[0], bytes_accessed=cost[1], transcendentals=cost[2]),
        name=name,
    )(scalars, *args)


def over(x, axis, bit):
    return lax.ppermute(x, axis, [(i, i ^ bit) for i in range(lax.axis_size(axis))])


def gather_pair(first, second):
    fx, sy = over(first, "tp", 1), over(second, "tp", 2)
    fy, sx = over(first, "tp", 2), over(second, "tp", 1)
    return (first, fx, fy, over(fx, "tp", 2)), (second, sx, sy, over(sy, "tp", 1))


def add(a, b):
    return a.astype(F32) + b.astype(F32)


def scatter_pair(parts):
    keep_a, near_a, keep_b, near_b, send_a, send_b = parts
    got_a, got_b = over(send_a, "tp", 2), over(send_b, "tp", 1)
    far_a = over(add(near_a, got_a[1]).astype(BF16), "tp", 1)
    far_b = over(add(near_b, got_b[1]).astype(BF16), "tp", 2)
    return add(keep_a, got_a[0]) + far_a.astype(F32), add(keep_b, got_b[0]) + far_b.astype(F32)


def emit_shapes(rows, width, tp):
    if tp == 4:
        half = rows // 2
        flat = [jax.ShapeDtypeStruct((half, width), BF16)] * 4
        return flat + [jax.ShapeDtypeStruct((2, half, width), BF16)] * 2
    return [jax.ShapeDtypeStruct((rows, width * tp), BF16)]


def emit_specs(rows, width, tp, step):
    if tp == 4:
        return [whole(s.shape) for s in emit_shapes(rows, width, tp)]
    return [pl.BlockSpec((rows, width), lambda i, s: (0, step(i)))]


def emit(outs, index, part, tp):
    if tp != 4:
        outs[0][...] = part
        return
    keep_a, near_a, keep_b, near_b, send_a, send_b = outs
    half = part.shape[0] // 2
    top, low = part[:half], part[half:]

    @pl.when(index == 0)
    def _():
        keep_a[...] = top
        keep_b[...] = low

    @pl.when(index == 1)
    def _():
        near_a[...] = top
        send_b[0] = low

    @pl.when(index == 2)
    def _():
        send_a[0] = top
        near_b[...] = low

    @pl.when(index == 3)
    def _():
        send_a[1] = top
        send_b[1] = low


def assemble(blocks, gain_ref, out_ref, tp_place):
    base = 0
    for pieces in blocks:
        rows = pieces[0].shape[0]
        width = pieces[0].shape[1]
        total = None
        for ref in pieces:
            values = ref[...].astype(F32)
            square = jnp.sum(values * values, axis=1, keepdims=True)
            total = square if total is None else total + square
        scale = lax.rsqrt(total / (width * len(pieces)) + EPS)
        for far, ref in enumerate(pieces):
            if len(pieces) == 1:
                cols = pl.ds(0, width)
            else:
                cols = pl.ds(pl.multiple_of((tp_place ^ far) * width, width), width)
            values = ref[...].astype(F32) * scale * gain_ref[:, cols].astype(F32)
            out_ref[base : base + rows, cols] = values.astype(BF16)
        base += rows


def expert_kernel(place, *refs, sizes, n_hidden, tp):
    count = sum(sizes)
    pieces, (gain, w_gate, w_up, w_down) = refs[:count], refs[count : count + 4]
    outs, (normed, hidden) = refs[count + 4 : -2], refs[-2:]
    step = pl.program_id(0)
    block = w_gate.shape[2]

    @pl.when(step == 0)
    def _():
        blocks, at = [], 0
        for size in sizes:
            blocks.append(pieces[at : at + size])
            at += size
        assemble(blocks, gain, normed, place[1])

    @pl.when(step < n_hidden)
    def _():
        gate = dot(normed[...], w_gate[0])
        up = dot(normed[...], w_up[0])
        value = (gate * jax.nn.sigmoid(gate) * up).astype(BF16)
        if n_hidden == 1:
            hidden[...] = value
        else:
            hidden[:, pl.ds(pl.multiple_of(step * block, block), block)] = value

    @pl.when(step >= n_hidden)
    def _():
        emit(outs, step - n_hidden, dot(hidden[...], w_down[0]).astype(BF16), tp)


def experts(place, blocks, gain, w_gate, w_up, w_down, tp, name):
    width_all, hidden_width = w_gate.shape[1], w_gate.shape[2]
    width = width_all // tp
    rows = sum(b[0].shape[0] for b in blocks)
    block = 256 if hidden_width % 256 == 0 else hidden_width
    n_hidden = hidden_width // block
    flat = [p for b in blocks for p in b]

    def down(i):
        return jnp.maximum(i - n_hidden, 0)

    def down_at(i, s):
        return (0, 0, (s[1] ^ down(i)) if tp == 4 else down(i))

    def up_at(i, s):
        return (0, 0, jnp.minimum(i, n_hidden - 1))

    return call(
        functools.partial(expert_kernel, sizes=tuple(len(b) for b in blocks), n_hidden=n_hidden, tp=tp),
        place,
        (n_hidden + tp,),
        [whole(p.shape) for p in flat]
        + [
            whole(gain.shape),
            pl.BlockSpec((1, width_all, block), up_at),
            pl.BlockSpec((1, width_all, block), up_at),
            pl.BlockSpec((1, hidden_width, width), down_at),
        ],
        emit_specs(rows, width, tp, down),
        emit_shapes(rows, width, tp),
        [pltpu.VMEM((rows, width_all), BF16), pltpu.VMEM((rows, hidden_width), BF16)],
        (6 * rows * width_all * hidden_width, 6 * width_all * hidden_width, rows * hidden_width),
        name,
        (*flat, gain, w_gate, w_up, w_down),
    )


def dispatch_kernel(place, own_meta, far_meta, own_rows, far_rows, *outs, capacity):
    chips = len(outs)
    tokens = own_rows.shape[0]
    z, core = place[0] // 2, place[0] % 2
    meta = jnp.concatenate([own_meta[...], far_meta[...]], axis=1)
    first, second = meta[0:1].astype(jnp.int32), meta[1:2].astype(jnp.int32)
    named = []
    for far in range(chips):
        expert = (z ^ far) * 2 + core
        named.append(((first == expert) | (second == expert)).astype(F32))
    spare = -chips % 8
    if spare:
        named.append(jnp.zeros((spare, 2 * tokens), F32))
    named = jnp.concatenate(named, axis=0)
    row = lax.broadcasted_iota(jnp.int32, (tokens, tokens), 0)
    col = lax.broadcasted_iota(jnp.int32, (tokens, tokens), 1)
    before = (row < col).astype(F32).astype(BF16)
    marks = named.astype(BF16)
    rank = jnp.concatenate([dot(marks[:, :tokens], before), dot(marks[:, tokens:], before) + capacity], axis=1)
    spot = jnp.where(named > 0, rank, -1.0).astype(jnp.int32)
    slot = lax.broadcasted_iota(jnp.int32, (2 * capacity, 2 * tokens), 0)
    picks = jnp.concatenate([(slot == spot[far : far + 1]).astype(F32).astype(BF16) for far in range(chips)], axis=0)
    rows = jnp.concatenate([own_rows[...], far_rows[...]], axis=0)
    slots = dot(picks, rows).astype(BF16)
    for far in range(chips):
        outs[far][...] = slots[far * 2 * capacity : (far + 1) * 2 * capacity]


def combine_kernel(place, own_meta, far_meta, *refs, capacity):
    chips = len(refs) - 2
    results, outs = refs[:chips], refs[chips:]
    tokens = own_meta.shape[0]
    z, core = place[0] // 2, place[0] % 2
    lane = lax.broadcasted_iota(jnp.int32, (1, 128), 1)
    expert = jnp.where(lane < chips, (z ^ lane) * 2 + core, -1)
    row = lax.broadcasted_iota(jnp.int32, (tokens, tokens), 0)
    col = lax.broadcasted_iota(jnp.int32, (tokens, tokens), 1)
    before = (col < row).astype(F32).astype(BF16)
    slot = lax.broadcasted_iota(jnp.int32, (tokens, chips * 2 * capacity), 1)
    rows = jnp.concatenate([ref[...] for ref in results], axis=0)
    for source, meta in enumerate((own_meta, far_meta)):
        values = meta[...]
        hits = [values[:, j : j + 1].astype(jnp.int32) == expert for j in range(2)]
        rank = dot(before, (hits[0] | hits[1]).astype(F32).astype(BF16))
        spots = rank + (lane * (2 * capacity) + source * capacity + 1).astype(F32)
        total = None
        for j in range(2):
            spot = jnp.sum(jnp.where(hits[j], spots, 0.0), axis=1, keepdims=True).astype(jnp.int32) - 1
            pick = dot((slot == spot).astype(F32).astype(BF16), rows) * values[:, 2 + j : 3 + j]
            total = pick if total is None else total + pick
        outs[source][...] = total.astype(outs[source].dtype)


def mixer_kernel(place, *refs, sizes):
    count = sum(sizes)
    pieces, rest = refs[:count], refs[count:]
    gain, w_query, w_forget, w_input, w_outgate, gap, extra, local_out, query_out, gate_out, state_out, normed = rest
    step = pl.program_id(0)
    length = normed.shape[0]
    span = w_query.shape[1]
    dim = state_out.shape[2]
    heads = span // dim

    @pl.when(step == 0)
    def _():
        blocks, at = [], 0
        for size in sizes:
            blocks.append(pieces[at : at + size])
            at += size
        assemble(blocks, gain, normed, place[1])

    x = normed[...]
    query = dot(x, w_query[...])
    query = query * jax.nn.sigmoid(query)
    key = gap[...] * jax.nn.sigmoid(-dot(x, w_forget[...]))
    value = dot(x, w_input[...]).astype(BF16)
    outgate = dot(x, w_outgate[...])
    gate_out[...] = outgate * jax.nn.sigmoid(outgate)
    decays = []
    for h in range(heads):
        decays.append(jnp.broadcast_to(extra[0, :, h : h + 1], (length, dim)))
    log_forget = jnp.log1p(-key) + (jnp.concatenate(decays, axis=1) if heads > 1 else decays[0])
    row = lax.broadcasted_iota(jnp.int32, (BLOCK, BLOCK), 0)
    col = lax.broadcasted_iota(jnp.int32, (BLOCK, BLOCK), 1)
    causal = col <= row
    lower = causal.astype(F32)
    state = [None] * heads
    passed = jnp.zeros((1, span), F32)
    for at in range(0, length, BLOCK):
        part = slice(at, at + BLOCK)
        running = dot(lower, log_forget[part], precision=lax.Precision.HIGHEST)
        last = running[BLOCK - 1 : BLOCK]
        middle = running[BLOCK // 2 - 1 : BLOCK // 2]
        q, k = query[part], key[part]
        inner = jnp.exp(running)
        q_local = (q * jnp.exp(running - middle)).astype(BF16)
        k_local = (k * jnp.exp(middle - running)).astype(BF16)
        q_state = q * inner
        k_state = (k * jnp.exp(last - running)).astype(BF16)
        query_out[part, :] = (q_state * jnp.exp(passed)).astype(BF16)
        q_state = q_state.astype(BF16)
        shrink = jnp.exp(last)
        for h in range(heads):
            own = slice(h * dim, (h + 1) * dim)
            v = value[part, own]
            scores = jnp.where(causal, dot(q_local[:, own], k_local[:, own], ((1,), (1,))), 0.0)
            out = dot(scores.astype(BF16), v)
            fresh = dot(v, k_state[:, own], ((0,), (0,)))
            if state[h] is not None:
                out = out + dot(q_state[:, own], state[h].astype(BF16), ((1,), (1,)))
                fresh = fresh + state[h] * shrink[:, own]
            state[h] = fresh
            local_out[part, own] = out
        passed = passed + last
    total = jnp.exp(passed)
    for h in range(heads):
        state_out[0, h * dim : (h + 1) * dim, :] = state[h].astype(BF16)
    tail = [total[:, h * dim : (h + 1) * dim] for h in range(heads)] + [jnp.zeros((16 - heads, dim), F32)]
    state_out[0, span : span + 16, :] = jnp.concatenate(tail, axis=0).astype(BF16)


def chain_states(earlier, later, dim):
    return [
        (d * s[0] + t, d * s[1]) for s, (t, d) in zip(earlier, later)
    ]


def read_pack(ref, step, heads, dim):
    states = []
    base = heads * dim
    tail = ref[step, base : base + 16, :].astype(F32)
    for h in range(heads):
        states.append((ref[step, h * dim : (h + 1) * dim, :].astype(F32), tail[h : h + 1]))
    return states


def chip_state_kernel(place, own, far, out):
    steps, rows, dim = own.shape
    heads = (rows - 16) // dim
    first = place[0] % 2 == 0
    for step in range(steps):
        a, b = read_pack(own, step, heads, dim), read_pack(far, step, heads, dim)
        tail = []
        for h in range(heads):
            s0, d0 = jnp.where(first, a[h][0], b[h][0]), jnp.where(first, a[h][1], b[h][1])
            s1, d1 = jnp.where(first, b[h][0], a[h][0]), jnp.where(first, b[h][1], a[h][1])
            out[step, h * dim : (h + 1) * dim, :] = (d1 * s0 + s1).astype(BF16)
            tail.append(d0 * d1)
        tail.append(jnp.zeros((16 - heads, dim), F32))
        out[step, heads * dim : heads * dim + 16, :] = jnp.concatenate(tail, axis=0).astype(BF16)


def mixout_kernel(place, *refs, packs, tp):
    past, (far, local_out, query, gate, gain, weight) = refs[:packs], refs[packs : packs + 6]
    outs, gated = refs[packs + 6 : -1], refs[-1]
    step = pl.program_id(0)
    steps, rows, dim = far.shape
    heads = (rows - 16) // dim

    @pl.when(step == 0)
    def _():
        second = place[0] % 2 == 1
        for part in range(steps):
            entering = [jnp.zeros((dim, dim), F32)] * heads
            for ref in past:
                pack = read_pack(ref, part, heads, dim)
                entering = [d * s + t for s, (t, d) in zip(entering, pack)]
            pack = read_pack(far, part, heads, dim)
            for h in range(heads):
                t, d = pack[h]
                start = jnp.where(second, d * entering[h] + t, entering[h]).astype(BF16)
                own = slice((part * heads + h) * dim, (part * heads + h + 1) * dim)
                out = local_out[:, own] + dot(query[:, own], start, ((1,), (1,)))
                scale = lax.rsqrt(jnp.mean(out * out, axis=1, keepdims=True) + EPS)
                gated[:, own] = (out * scale * gain[...].astype(F32) * gate[:, own]).astype(BF16)

    emit(outs, step, dot(gated[...], weight[...]).astype(BF16), tp)


def per_device(
    mix_rows,
    mix_gain,
    w_query,
    w_forget,
    w_input,
    w_outgate,
    forget_gap,
    decay_extra,
    head_gain,
    w_mixout,
    moe_rows,
    moe_gain,
    route_ids,
    route_scores,
    w_gate,
    w_up,
    w_down,
):
    ep, tp = lax.axis_size("ep"), lax.axis_size("tp")
    chips = ep // 2
    tokens, top = route_ids.shape
    width = moe_rows.shape[1]
    width_all = width * tp
    capacity = tokens * top * 3 // (2 * ep)
    slots = 2 * capacity
    place = jnp.stack([lax.axis_index("ep"), lax.axis_index("tp")]).astype(jnp.int32)
    block = functools.partial(jax.ShapeDtypeStruct, dtype=BF16)

    weights = route_scores / jnp.sum(route_scores, axis=1, keepdims=True)
    meta = jnp.concatenate([route_ids.astype(F32), weights], axis=1)
    meta_t = meta.T
    far_rows = over(moe_rows, "ep", 1)
    far_meta_t = over(meta_t, "ep", 1)

    half = mix_rows.shape[0] // 2
    if tp == 4:
        mix_blocks = gather_pair(mix_rows[:half], mix_rows[half:])
    else:
        mix_blocks = ((lax.all_gather(mix_rows, "tp", axis=1, tiled=True),),)

    sent = call(
        functools.partial(dispatch_kernel, capacity=capacity),
        place,
        (1,),
        [whole(meta_t.shape)] * 2 + [whole(moe_rows.shape)] * 2,
        [whole((slots, width))] * chips,
        [block((slots, width))] * chips,
        [],
        (4 * chips * slots * tokens * width * 2, 8 * tokens * width, 0),
        "dispatch",
        (meta_t, far_meta_t, moe_rows, far_rows),
    )
    arrived = [sent[0]] + [over(sent[far], "ep", 2 * far) for far in range(1, chips)]

    length = mix_rows.shape[0]
    local_width = w_query.shape[1]
    dim = head_gain.shape[0]
    span = min(2 * dim, local_width)
    steps = local_width // span
    heads = span // dim
    extra = decay_extra.reshape(steps, heads, length).transpose(0, 2, 1)
    flat = [p for b in mix_blocks for p in b]
    wide = pl.BlockSpec((width_all, span), lambda i, s: (0, i))
    strip = pl.BlockSpec((length, span), lambda i, s: (0, i))
    local_out, query, gate, pack = call(
        functools.partial(mixer_kernel, sizes=tuple(len(b) for b in mix_blocks)),
        place,
        (steps,),
        [whole(p.shape) for p in flat]
        + [whole((1, width_all))]
        + [wide] * 4
        + [pl.BlockSpec((1, span), lambda i, s: (0, i)), pl.BlockSpec((1, length, heads), lambda i, s: (i, 0, 0))],
        [strip, strip, strip, pl.BlockSpec((1, span + 16, dim), lambda i, s: (i, 0, 0))],
        [
            jax.ShapeDtypeStruct((length, local_width), F32),
            block((length, local_width)),
            jax.ShapeDtypeStruct((length, local_width), F32),
            block((steps, span + 16, dim)),
        ],
        [pltpu.VMEM((length, width_all), BF16)],
        (8 * length * width_all * local_width, 8 * width_all * local_width, 8 * length * local_width),
        "mixer",
        (*flat, mix_gain[None], w_query, w_forget, w_input, w_outgate, forget_gap[None], extra),
    )
    far_pack = over(pack, "ep", 1)
    chip_pack = call(
        chip_state_kernel,
        place,
        (1,),
        [whole(pack.shape)] * 2,
        whole(pack.shape),
        block(pack.shape),
        [],
        (4 * pack.size, 6 * pack.size, 0),
        "chip_state",
        (pack, far_pack),
    )
    past = [
        lax.ppermute(chip_pack, "ep", [(i, i + 2 * far) for i in range(ep - 2 * far)])
        for far in range(chips - 1, 0, -1)
    ]

    if tp == 4:
        pairs = [(far, far + 1) for far in range(0, chips, 2)]
        parts = []
        for pair in pairs:
            blocks = gather_pair(arrived[pair[0]], arrived[pair[1]])
            parts.append(experts(place, blocks, moe_gain[None], w_gate, w_up, w_down, tp, "experts"))
    else:
        joined = lax.all_gather(jnp.concatenate(arrived, axis=0), "tp", axis=1, tiled=True)
        parts = experts(place, ((joined,),), moe_gain[None], w_gate, w_up, w_down, tp, "experts")

    mixed = call(
        functools.partial(mixout_kernel, packs=len(past), tp=tp),
        place,
        (tp,),
        [whole(pack.shape)] * (len(past) + 1)
        + [whole((length, local_width))] * 3
        + [whole((1, dim)), pl.BlockSpec((local_width, width), lambda i, s: (0, (s[1] ^ i) if tp == 4 else i))],
        emit_specs(length, width, tp, lambda i: i),
        emit_shapes(length, width, tp),
        [pltpu.VMEM((length, local_width), BF16)],
        (2 * length * width_all * local_width, 2 * width_all * local_width, length),
        "mixout",
        (*past, far_pack, local_out, query, gate, head_gain[None], w_mixout),
    )

    if tp == 4:
        mix_out = jnp.concatenate(scatter_pair(mixed), axis=0).astype(BF16)
        results = [None] * chips
        for pair, part in reversed(list(zip(pairs, parts))):
            for far, value in zip(pair, scatter_pair(part)):
                value = value.astype(BF16)
                results[far] = over(value, "ep", 2 * far) if far else value
    else:
        mix_out = lax.psum_scatter(mixed[0], "tp", scatter_dimension=1, tiled=True)
        summed = lax.psum_scatter(parts[0], "tp", scatter_dimension=1, tiled=True)
        results = []
        for far in range(chips):
            value = summed[far * slots : (far + 1) * slots]
            results.append(over(value, "ep", 2 * far) if far else value)

    own, far = call(
        functools.partial(combine_kernel, capacity=capacity),
        place,
        (1,),
        [whole(meta.shape)] * 2 + [whole((slots, width))] * chips,
        [whole((tokens, width))] * 2,
        [jax.ShapeDtypeStruct((tokens, width), F32), block((tokens, width))],
        [],
        (8 * chips * slots * tokens * width, 2 * chips * slots * width, 0),
        "combine",
        (meta, far_meta_t.T, *results),
    )
    moe_out = add(own, over(far, "ep", 1)).astype(BF16)
    return (mix_out, moe_out)


def solution(mesh):
    placed = (
        P("ep", "tp"),
        P(),
        P(None, "tp"),
        P(None, "tp"),
        P(None, "tp"),
        P(None, "tp"),
        P("tp"),
        P("tp", "ep"),
        P(),
        P("tp", None),
        P("ep", "tp"),
        P(),
        P("ep", None),
        P("ep", None),
        P("ep", None, "tp"),
        P("ep", None, "tp"),
        P("ep", "tp", None),
    )
    return jax.shard_map(
        per_device,
        mesh=mesh,
        in_specs=placed,
        out_specs=(P("ep", "tp"), P("ep", "tp")),
        check_vma=False,
    )
```

```python
import functools

import jax
import jax.numpy as jnp
from jax import lax
from jax.experimental import pallas as pl
from jax.experimental.pallas import tpu as pltpu
from jax.sharding import PartitionSpec as P


BLOCK = 64
EPS = 1e-06
F32 = jnp.float32
BF16 = jnp.bfloat16


def dot(a, b, dims=((1,), (0,)), precision=None):
    return lax.dot_general(a, b, (dims, ((), ())), precision=precision, preferred_element_type=F32)


def call(kernel, place, out_shape, scratch, cost, args, far_off=()):
    return pl.pallas_call(
        kernel,
        in_specs=[pl.BlockSpec(memory_space=pltpu.SMEM)] + [
            pl.BlockSpec(memory_space=pltpu.HBM if n in far_off else pltpu.VMEM) for n in range(len(args))
        ],
        out_specs=[pl.BlockSpec(memory_space=pltpu.VMEM)] * len(out_shape),
        out_shape=out_shape,
        scratch_shapes=scratch,
        compiler_params=pltpu.CompilerParams(vmem_limit_bytes=24 * 1024 * 1024),
        cost_estimate=pl.CostEstimate(flops=cost[0], bytes_accessed=cost[1], transcendentals=cost[2]),
    )(place, *args)


def over(x, axis, bit):
    return lax.ppermute(x, axis, [(i, i ^ bit) for i in range(lax.axis_size(axis))])


def gather_pair(first, second):
    fx, sy = over(first, "tp", 1), over(second, "tp", 2)
    fy, sx = over(first, "tp", 2), over(second, "tp", 1)
    return (first, fx, fy, over(fx, "tp", 2)), (second, sx, sy, over(sy, "tp", 1))


def add(a, b):
    return a.astype(F32) + b.astype(F32)


def scatter_pair(parts):
    keep_a, near_a, keep_b, near_b, send_a, send_b = parts
    got_a, got_b = over(send_a, "tp", 2), over(send_b, "tp", 1)
    far_a = over(add(near_a, got_a[1]).astype(BF16), "tp", 1)
    far_b = over(add(near_b, got_b[1]).astype(BF16), "tp", 2)
    return add(keep_a, got_a[0]) + far_a.astype(F32), add(keep_b, got_b[0]) + far_b.astype(F32)


def emit_shapes(rows, width, tp):
    if tp == 4:
        half = rows // 2
        flat = [jax.ShapeDtypeStruct((half, width), BF16)] * 4
        return flat + [jax.ShapeDtypeStruct((2, half, width), BF16)] * 2
    return [jax.ShapeDtypeStruct((rows, width * tp), BF16)]


def emit(outs, value, weight, place, tp):
    width = weight.shape[-1] // tp
    if tp != 4:
        for far in range(tp):
            cols = slice(far * width, (far + 1) * width)
            outs[0][:, cols] = dot(value, weight[:, cols]).astype(BF16)
        return
    keep_a, near_a, keep_b, near_b, send_a, send_b = outs
    half = value.shape[0] // 2
    spots = (
        (keep_a, keep_b),
        (near_a, send_b.at[0]),
        (send_a.at[0], near_b),
        (send_a.at[1], send_b.at[1]),
    )
    for far, (top, low) in enumerate(spots):
        cols = pl.ds(pl.multiple_of((place[1] ^ far) * width, width), width)
        part = dot(value, weight[:, cols]).astype(BF16)
        top[...] = part[:half]
        low[...] = part[half:]


def assemble(refs, plan, gain_ref, out_ref, tp_place):
    base = 0
    for rows, pieces in plan:
        width = refs[0].shape[1]
        total = None
        for index, at in pieces:
            values = refs[index][at : at + rows].astype(F32)
            square = jnp.sum(values * values, axis=1, keepdims=True)
            total = square if total is None else total + square
        scale = lax.rsqrt(total / (width * len(pieces)) + EPS)
        for far, (index, at) in enumerate(pieces):
            if len(pieces) == 1:
                cols = pl.ds(0, width)
            else:
                cols = pl.ds(pl.multiple_of((tp_place ^ far) * width, width), width)
            values = refs[index][at : at + rows].astype(F32) * scale * gain_ref[:, cols].astype(F32)
            out_ref[base : base + rows, cols] = values.astype(BF16)
        base += rows


def expert_kernel(place, *refs, plan, block, tp):
    count = len(refs) - 6 - (6 if tp == 4 else 1)
    pieces, (gain, w_gate, w_up, w_down) = refs[:count], refs[count : count + 4]
    outs, (normed, hidden) = refs[count + 4 : -2], refs[-2:]
    assemble(pieces, plan, gain, normed, place[1])
    x = normed[...]
    for at in range(0, hidden.shape[1], block):
        cols = slice(at, at + block)
        gate = dot(x, w_gate[0, :, cols])
        up = dot(x, w_up[0, :, cols])
        hidden[:, cols] = (gate * jax.nn.sigmoid(gate) * up).astype(BF16)
    emit(outs, hidden[...], w_down.at[0], place, tp)


def experts(place, blocks, gain, w_gate, w_up, w_down, tp):
    width_all, hidden_width = w_gate.shape[1], w_gate.shape[2]
    rows = sum(b[0].shape[0] for b in blocks)
    block = 256 if hidden_width % 256 == 0 else hidden_width
    flat, plan = [p for b in blocks for p in b], []
    for b in blocks:
        first = sum(len(pieces) for _, pieces in plan)
        plan.append((b[0].shape[0], [(first + i, 0) for i in range(len(b))]))
    return call(
        functools.partial(expert_kernel, plan=plan, block=block, tp=tp),
        place,
        emit_shapes(rows, width_all // tp, tp),
        [pltpu.VMEM((rows, width_all), BF16), pltpu.VMEM((rows, hidden_width), BF16)],
        (6 * rows * width_all * hidden_width, 6 * width_all * hidden_width, rows * hidden_width),
        (*flat, gain, w_gate, w_up, w_down),
    )


def dispatch_kernel(place, own_ids, far_ids, own_rows, far_rows, *refs, capacity):
    outs, (ids, rows, sems) = refs[:-3], refs[-3:]
    chips = len(outs)
    tokens = own_rows.shape[0]
    ids_copy = pltpu.make_async_copy(own_ids, ids, sems.at[0])
    rows_copy = pltpu.make_async_copy(own_rows, rows.at[pl.ds(0, tokens)], sems.at[1])
    ids_copy.start()
    rows_copy.start()
    rows[tokens:] = far_rows[...]
    row = lax.broadcasted_iota(jnp.int32, (tokens, tokens), 0)
    col = lax.broadcasted_iota(jnp.int32, (tokens, tokens), 1)
    before = (row < col).astype(F32).astype(BF16)
    z, core = place[0] // 2, place[0] % 2
    ids_copy.wait()
    both = jnp.concatenate([ids[...], far_ids[...]], axis=1)
    first, second = both[0:1], both[1:2]
    named = []
    for far in range(chips):
        expert = (z ^ far) * 2 + core
        named.append(((first == expert) | (second == expert)).astype(F32))
    spare = -chips % 8
    if spare:
        named.append(jnp.zeros((spare, 2 * tokens), F32))
    named = jnp.concatenate(named, axis=0)
    marks = named.astype(BF16)
    rank = jnp.concatenate([dot(marks[:, :tokens], before), dot(marks[:, tokens:], before) + capacity], axis=1)
    spot = jnp.where(named > 0, rank, -1.0).astype(jnp.int32)
    slot = lax.broadcasted_iota(jnp.int32, (2 * capacity, 2 * tokens), 0)
    picks = jnp.concatenate([(slot == spot[far : far + 1]).astype(F32).astype(BF16) for far in range(chips)], axis=0)
    rows_copy.wait()
    slots = dot(picks, rows[...]).astype(BF16)
    for far in range(chips):
        outs[far][...] = slots[far * 2 * capacity : (far + 1) * 2 * capacity]


def plan_kernel(place, own_ids, far_ids, own_scores, far_scores, *outs, chips, capacity):
    tokens = own_ids.shape[1]
    z, core = place[0] // 2, place[0] % 2
    lane = lax.broadcasted_iota(jnp.int32, (1, 128), 1)
    expert = jnp.where(lane < chips, (z ^ lane) * 2 + core, -1)
    row = lax.broadcasted_iota(jnp.int32, (tokens, tokens), 0)
    col = lax.broadcasted_iota(jnp.int32, (tokens, tokens), 1)
    before = (col < row).astype(F32).astype(BF16)
    slot = lax.broadcasted_iota(jnp.int32, (tokens, chips * 2 * capacity), 1)
    for source, (ids, scores) in enumerate(((own_ids, own_scores), (far_ids, far_scores))):
        weights = scores[...] / jnp.sum(scores[...], axis=0, keepdims=True)
        values = jnp.concatenate([ids[...].astype(F32), weights, jnp.zeros((4, tokens), F32)], axis=0).T
        hits = [values[:, j : j + 1].astype(jnp.int32) == expert for j in range(2)]
        rank = dot(before, (hits[0] | hits[1]).astype(F32).astype(BF16))
        spots = rank + (lane * (2 * capacity) + source * capacity + 1).astype(F32)
        mix = None
        for j in range(2):
            spot = jnp.sum(jnp.where(hits[j], spots, 0.0), axis=1, keepdims=True).astype(jnp.int32) - 1
            part = jnp.where(slot == spot, values[:, 2 + j : 3 + j], 0.0)
            mix = part if mix is None else mix + part
        outs[source][...] = mix.astype(BF16)


def combine_kernel(place, mix, *refs):
    results, out = refs[:-1], refs[-1]
    rows = jnp.concatenate([ref[...] for ref in results], axis=0)
    out[...] = dot(mix[...], rows).astype(out.dtype)


def mixer_kernel(place, *refs, plan, number):
    if plan:
        count = len(refs) - 12
        pieces, gain, refs = refs[:count], refs[count], refs[count + 1 :]
        normed = refs[-1]
        assemble(pieces, plan, gain, normed, place[1])
        w_query, w_forget, w_input, w_outgate, gap, extra, local_out, query_out, gate_out, state_out, _ = refs
    else:
        normed, w_query, w_forget, w_input, w_outgate, gap, extra, local_out, query_out, gate_out, state_out = refs
    length, span = local_out.shape
    dim = state_out.shape[1]
    heads = span // dim
    here = slice(number * span, (number + 1) * span)

    x = normed[...]
    query = dot(x, w_query[:, here])
    query = query * jax.nn.sigmoid(query)
    key = gap[:, here] * jax.nn.sigmoid(-dot(x, w_forget[:, here]))
    value = dot(x, w_input[:, here]).astype(BF16)
    outgate = dot(x, w_outgate[:, here])
    gate_out[...] = outgate * jax.nn.sigmoid(outgate)
    decays = []
    extras = extra[...]
    if extras.shape[0] % 8:
        extras = jnp.concatenate([extras, jnp.zeros((-extras.shape[0] % 8, length), F32)], axis=0)
    extras = extras.T
    for h in range(heads):
        at = number * heads + h
        decays.append(jnp.broadcast_to(extras[:, at : at + 1], (length, dim)))
    log_forget = jnp.log1p(-key) + (jnp.concatenate(decays, axis=1) if heads > 1 else decays[0])
    row = lax.broadcasted_iota(jnp.int32, (BLOCK, BLOCK), 0)
    col = lax.broadcasted_iota(jnp.int32, (BLOCK, BLOCK), 1)
    causal = col <= row
    lower = causal.astype(F32)
    state = [None] * heads
    passed = jnp.zeros((1, span), F32)
    for at in range(0, length, BLOCK):
        part = slice(at, at + BLOCK)
        running = dot(lower, log_forget[part], precision=lax.Precision.HIGHEST)
        end = running[BLOCK - 1 : BLOCK]
        middle = running[BLOCK // 2 - 1 : BLOCK // 2]
        q, k = query[part], key[part]
        q_local = (q * jnp.exp(running - middle)).astype(BF16)
        k_local = (k * jnp.exp(middle - running)).astype(BF16)
        q_state = q * jnp.exp(running)
        k_state = (k * jnp.exp(end - running)).astype(BF16)
        query_out[part, :] = (q_state * jnp.exp(passed)).astype(BF16)
        q_state = q_state.astype(BF16)
        shrink = jnp.exp(end)
        for h in range(heads):
            own = slice(h * dim, (h + 1) * dim)
            v = value[part, own]
            scores = jnp.where(causal, dot(q_local[:, own], k_local[:, own], ((1,), (1,))), 0.0)
            out = dot(scores.astype(BF16), v)
            fresh = dot(v, k_state[:, own], ((0,), (0,)))
            if state[h] is not None:
                out = out + dot(q_state[:, own], state[h].astype(BF16), ((1,), (1,)))
                fresh = fresh + state[h] * shrink[:, own]
            state[h] = fresh
            local_out[part, own] = out
        passed = passed + end
    total = jnp.exp(passed)
    write_pack(state_out, [(state[h], total[:, h * dim : (h + 1) * dim]) for h in range(heads)])


def write_pack(ref, pairs):
    dim = ref.shape[1]
    for h, (state, _) in enumerate(pairs):
        ref[h * dim : (h + 1) * dim, :] = state.astype(BF16)
    tail = [decay for _, decay in pairs] + [jnp.zeros((16 - len(pairs), dim), F32)]
    ref[len(pairs) * dim :, :] = jnp.concatenate(tail, axis=0).astype(BF16)


def read_pack(ref):
    rows, dim = ref.shape
    heads = (rows - 16) // dim
    tail = ref[heads * dim :, :].astype(F32)
    return [(ref[h * dim : (h + 1) * dim, :].astype(F32), tail[h : h + 1]) for h in range(heads)]


def follow(earlier, later):
    return [(d * s + t, d * c) for (s, c), (t, d) in zip(earlier, later)]


def choose(flag, yes, no):
    return [tuple(jnp.where(flag, a, b) for a, b in zip(x, y)) for x, y in zip(yes, no)]


def scan_kernel(place, own, far, *refs, bit, count):
    before, outs = refs[:-2], refs[-2:]
    second = (place[0] & bit) != 0
    a, b = [], []
    for n in range(count):
        a += read_pack(own.at[n] if count > 1 else own)
        b += read_pack(far.at[n] if count > 1 else far)
    totals = choose(second, follow(b, a), follow(a, b))
    if before:
        past = []
        for n in range(count):
            past += read_pack(before[0].at[n] if count > 1 else before[0])
        entering = choose(second, follow(b, past), past)
    else:
        entering = choose(second, b, [(jnp.zeros_like(s), jnp.ones_like(d)) for s, d in b])
    per = len(totals) // count
    for out, values in zip(outs, (totals, entering)):
        for n in range(count):
            write_pack(out.at[n] if count > 1 else out, values[n * per : (n + 1) * per])


def mixout_kernel(place, *refs, count, bit, tp):
    past, far, gain, weight = refs[:4]
    parts, outs, gated = refs[4 : 4 + 3 * count], refs[4 + 3 * count : -1], refs[-1]
    second = (place[0] & bit) != 0
    for n in range(count):
        local_out, query, gate = parts[n], parts[count + n], parts[2 * count + n]
        before = read_pack(past.at[n] if count > 1 else past)
        added = read_pack(far.at[n] if count > 1 else far)
        entering = choose(second, follow(added, before), before)
        dim = entering[0][0].shape[0]
        for h, (state, _) in enumerate(entering):
            own = slice(h * dim, (h + 1) * dim)
            out = local_out[:, own] + dot(query[:, own], state.astype(BF16), ((1,), (1,)))
            scale = lax.rsqrt(jnp.mean(out * out, axis=1, keepdims=True) + EPS)
            at = n * local_out.shape[1] + h * dim
            gated[:, at : at + dim] = (out * scale * gain[...].astype(F32) * gate[:, own]).astype(BF16)
    emit(outs, gated[...], weight, place, tp)


def per_device(
    mix_rows,
    mix_gain,
    w_query,
    w_forget,
    w_input,
    w_outgate,
    forget_gap,
    decay_extra,
    head_gain,
    w_mixout,
    moe_rows,
    moe_gain,
    route_ids,
    route_scores,
    w_gate,
    w_up,
    w_down,
):
    ep, tp = lax.axis_size("ep"), lax.axis_size("tp")
    chips = ep // 2
    tokens, top = route_ids.shape
    width = moe_rows.shape[1]
    width_all = width * tp
    capacity = tokens * top * 3 // (2 * ep)
    slots = 2 * capacity
    place = jnp.stack([lax.axis_index("ep"), lax.axis_index("tp")]).astype(jnp.int32)
    block = functools.partial(jax.ShapeDtypeStruct, dtype=BF16)

    ids, scores = route_ids.T, route_scores.T
    far_ids = over(ids, "ep", 1)
    far_rows = over(moe_rows, "ep", 1)
    far_scores = over(scores, "ep", 1)

    half = mix_rows.shape[0] // 2
    if tp == 4:
        by_x, by_y = over(mix_rows, "tp", 1), over(mix_rows, "tp", 2)
        flat = [mix_rows, by_x, by_y, over(by_x[:half], "tp", 2), over(by_y[half:], "tp", 1)]
        plan = [(half, [(0, 0), (1, 0), (2, 0), (3, 0)]), (half, [(0, half), (1, half), (2, half), (4, 0)])]
    else:
        flat, plan = [lax.all_gather(mix_rows, "tp", axis=1, tiled=True)], [(2 * half, [(0, 0)])]

    sent = call(
        functools.partial(dispatch_kernel, capacity=capacity),
        place,
        [block((slots, width))] * chips,
        [
            pltpu.VMEM(ids.shape, jnp.int32),
            pltpu.VMEM((2 * tokens, width), BF16),
            pltpu.SemaphoreType.DMA((2,)),
        ],
        (20_000_000_000, 8 * tokens * width, 0),
        (ids, far_ids, moe_rows, far_rows),
        (0, 2),
    )
    arrived = [sent[0]] + [over(sent[far], "ep", 2 * far) for far in range(1, chips)]

    own_mix, far_mix = call(
        functools.partial(plan_kernel, chips=chips, capacity=capacity),
        place,
        [block((tokens, chips * slots))] * 2,
        [],
        (8 * tokens * chips * slots, 4 * tokens * chips * slots, 0),
        (ids, far_ids, scores, far_scores),
    )

    length = mix_rows.shape[0]
    local_width = w_query.shape[1]
    dim = head_gain.shape[0]
    span = min(2 * dim, local_width)
    count = local_width // span
    locals_out, queries, gates, packs = [], [], [], []
    for n in range(count):
        first_in = flat + [mix_gain[None]] if n == 0 else [normed]
        out = call(
            functools.partial(mixer_kernel, plan=plan if n == 0 else None, number=n),
            place,
            [
                jax.ShapeDtypeStruct((length, span), F32),
                block((length, span)),
                jax.ShapeDtypeStruct((length, span), F32),
                block((span + 16, dim)),
            ]
            + [block((length, width_all))] * (n == 0),
            [],
            (8 * length * width_all * span, 8 * width_all * span, 8 * length * span),
            (*first_in, w_query, w_forget, w_input, w_outgate, forget_gap[None], decay_extra),
        )
        locals_out.append(out[0])
        queries.append(out[1])
        gates.append(out[2])
        packs.append(out[3])
        if n == 0:
            normed = out[4]
    total = jnp.stack(packs) if count > 1 else packs[0]
    entering, bit = None, 1
    while True:
        far_total = over(total, "ep", bit)
        if 2 * bit >= ep:
            break
        before = [] if entering is None else [entering]
        total, entering = call(
            functools.partial(scan_kernel, bit=bit, count=count),
            place,
            [block(total.shape)] * 2,
            [],
            (4 * total.size, 6 * total.size, 0),
            (total, far_total, *before),
        )
        bit *= 2

    if tp == 4:
        pairs = [(far, far + chips // 2) for far in range(chips // 2)]
        parts = []
        for pair in pairs:
            blocks = gather_pair(arrived[pair[0]], arrived[pair[1]])
            parts.append(experts(place, blocks, moe_gain[None], w_gate, w_up, w_down, tp))
    else:
        joined = lax.all_gather(jnp.concatenate(arrived, axis=0), "tp", axis=1, tiled=True)
        parts = experts(place, ((joined,),), moe_gain[None], w_gate, w_up, w_down, tp)

    mixed = call(
        functools.partial(mixout_kernel, count=count, bit=bit, tp=tp),
        place,
        emit_shapes(length, width, tp),
        [pltpu.VMEM((length, local_width), BF16)],
        (2 * length * width_all * local_width, 2 * width_all * local_width, length),
        (entering, far_total, head_gain[None], w_mixout, *locals_out, *queries, *gates),
    )

    if tp == 4:
        mix_out = jnp.concatenate(scatter_pair(mixed), axis=0).astype(BF16)
        results = [None] * chips
        for pair, part in zip(pairs, parts):
            for far, value in zip(pair, scatter_pair(part)):
                value = value.astype(BF16)
                results[far] = over(value, "ep", 2 * far) if far else value
    else:
        mix_out = lax.psum_scatter(mixed[0], "tp", scatter_dimension=1, tiled=True)
        summed = lax.psum_scatter(parts[0], "tp", scatter_dimension=1, tiled=True)
        results = []
        for far in range(chips):
            value = summed[far * slots : (far + 1) * slots]
            results.append(over(value, "ep", 2 * far) if far else value)

    def combine(mix, dtype):
        return call(
            combine_kernel,
            place,
            [jax.ShapeDtypeStruct((tokens, width), dtype)],
            [],
            (2 * mix.size * width, 2 * chips * slots * width, 0),
            (mix, *results),
        )[0]

    far = combine(far_mix, BF16)
    own = combine(own_mix, F32)
    moe_out = add(own, over(far, "ep", 1)).astype(BF16)
    return (mix_out, moe_out)


def solution(mesh):
    placed = (
        P("ep", "tp"),
        P(),
        P(None, "tp"),
        P(None, "tp"),
        P(None, "tp"),
        P(None, "tp"),
        P("tp"),
        P("tp", "ep"),
        P(),
        P("tp", None),
        P("ep", "tp"),
        P(),
        P("ep", None),
        P("ep", None),
        P("ep", None, "tp"),
        P("ep", None, "tp"),
        P("ep", "tp", None),
    )

    return jax.shard_map(
        per_device,
        mesh=mesh,
        in_specs=placed,
        out_specs=(P("ep", "tp"), P("ep", "tp")),
        check_vma=False,
    )
```
